32 devices in a mesh: sp: 8 (over z, y), tp: 4 (over x, core).
Axes of the slice: x: 2, y: 2, z: 4, core: 2. Of those that a mesh axis runs over, the one named last changes fastest.
Arguments:
- stream: bfloat16 [3072, 2048], P(('sp', 'tp')), may hold values from -6 to 6
- query_nope: bfloat16 [3072, 16, 128], P('sp', 'tp'), may hold values from -6 to 6
- query_rope: bfloat16 [3072, 16, 64], P('sp', 'tp'), may hold values from -700 to 700
- latent: bfloat16 [3072, 512], P('sp'), may hold values from -6 to 6
- rope_key: bfloat16 [3072, 64], P('sp'), may hold values from -6 to 6
- latent_gain: float32 [512], replicated, may hold values from 0.1 to 1.9
- key_up: bfloat16 [512, 16, 128], P(None, 'tp'), may hold values from -0.375 to 0.375
- value_up: bfloat16 [512, 16, 128], P(None, 'tp'), may hold values from -2.6516504 to 2.6516504
- out_gain: float32 [2048], P('tp'), may hold values from 0.1 to 1.9
- out_weight: bfloat16 [2048, 2048], P('tp'), may hold values from -0.125 to 0.125
- norm_gain: float32 [2048], replicated, may hold values from 0.1 to 1.9
- ff_in: bfloat16 [2048, 8192], P('sp', 'tp'), may hold values from -0.125 to 0.125
- ff_out: bfloat16 [8192, 2048], P('tp', 'sp'), may hold values from -0.0625 to 0.0625
Outputs:
- layer_out: bfloat16 [3072, 2048], P(('sp', 'tp'))
The draws below stay inside these ranges and needn't reach their ends.
All inputs are finite; a program needn't handle non-finite values.
Results may differ from the reference program's by a relative error of at most 0.018.
Values may be sent and summed in bfloat16 or wider, within the bound.
A program may use at most 128 MiB of HBM per device.

```python
import math
import jax
import jax.numpy as jnp
from jax import lax

D = 2048
FF = 8192
HEADS = 16
NOPE = 128
ROPE = 64
LATENT = 512
VDIM = 128
TOKENS = 3072


def draw_query_rope(key, part):
    base_draw = jax.random.normal(key, (TOKENS, HEADS, ROPE), jnp.float32)
    return jnp.clip(base_draw, -700.0, 700.0).astype(jnp.bfloat16)


def draw_value_up(key, part):
    base_draw = jnp.clip(jax.random.normal(key, (LATENT, HEADS, VDIM), jnp.float32), -6.0, 6.0) / jnp.sqrt(jnp.float32(LATENT))
    factor = jnp.power(4.0, jnp.arange(HEADS, dtype=jnp.float32) / max(HEADS - 1, 1))
    return (base_draw * factor[None, :, None]).astype(jnp.bfloat16)


def block_levels(rng, extent, split, low, largest):
    def one(axis_at, blocks):
        heights = jax.random.uniform(jax.random.fold_in(jax.random.fold_in(rng, 6), axis_at), (blocks,), jnp.float32, low / len(split), largest / len(split))
        return jnp.repeat(jnp.exp(heights), extent[axis_at] // blocks).reshape((-1,) + (1,) * (len(extent) - axis_at - 1))

    level = one(*split[0])
    for cut in split[1:]:
        level = level * one(*cut)
    return level


def scatter_about(key, shape, scale, reach, split=(), kind=jnp.bfloat16):
    entries = scale * jax.random.normal(key, shape, jnp.float32)
    if split:
        entries = entries * block_levels(key, shape, split, -0.22, 0.18)
    return jnp.clip(entries, -reach, reach).astype(kind)


def setup_inputs(seed: int = 0) -> dict:
    key_list = jax.random.split(jax.random.key(seed), 14)
    stream = scatter_about(key_list[0], (TOKENS, D), 1.0, 6.0, ((0, 32),))
    query_nope = scatter_about(key_list[1], (TOKENS, HEADS, NOPE), 1.0, 6.0, ((0, 8), (1, 4)))
    query_rope = draw_query_rope(jax.random.fold_in(key_list[13], 71), 0)
    latent = scatter_about(key_list[3], (TOKENS, LATENT), 1.0, 6.0, ((0, 8),))
    rope_key = scatter_about(key_list[4], (TOKENS, ROPE), 1.0, 6.0, ((0, 8),))
    latent_gain = jnp.clip(1.0 + 0.18 * jax.random.normal(key_list[5], (LATENT,), jnp.float32), 0.1, 1.9)
    key_up = scatter_about(key_list[6], (LATENT, HEADS, NOPE), (2 * NOPE) ** -0.5, 0.375, ((1, 4),))
    value_up = draw_value_up(jax.random.fold_in(key_list[13], 71), 0)
    out_gain = jnp.clip(1.0 + 0.18 * jax.random.normal(key_list[8], (HEADS * VDIM,), jnp.float32), 0.1, 1.9)
    out_weight = scatter_about(key_list[9], (HEADS * VDIM, D), (HEADS * VDIM) ** -0.5, 0.125, ((0, 4),))
    norm_gain = jnp.clip(1.0 + 0.18 * jax.random.normal(key_list[10], (D,), jnp.float32), 0.1, 1.9)
    ff_in = scatter_about(key_list[11], (D, FF), D ** -0.5, 0.125, ((0, 8), (1, 4)))
    ff_out = scatter_about(key_list[12], (FF, D), FF ** -0.5, 0.0625, ((0, 4), (1, 8)))
    return {"stream": stream, "query_nope": query_nope, "query_rope": query_rope, "latent": latent, "rope_key": rope_key, "latent_gain": latent_gain, "key_up": key_up, "value_up": value_up, "out_gain": out_gain, "out_weight": out_weight, "norm_gain": norm_gain, "ff_in": ff_in, "ff_out": ff_out}


EPS = 1e-06
THETA = 10000.0

def turn(values, positions):
    full_width = values.shape[-1]
    half_width = full_width // 2
    inverse = jnp.power(THETA, -jnp.arange(0, full_width, 2, dtype=jnp.float32) / full_width)
    angles = positions[:, None] * inverse[None, :]
    cosine = jnp.cos(angles)
    sine_part = jnp.sin(angles)
    if values.ndim == 3:
        cosine = cosine[:, None, :]
        sine_part = sine_part[:, None, :]
    vector = values.astype(jnp.float32)
    lower_half = vector[..., :half_width]
    upper_half = vector[..., half_width:]
    return jnp.concatenate([lower_half * cosine - upper_half * sine_part, lower_half * sine_part + upper_half * cosine], axis=-1)

def reference(stream, query_nope, query_rope, latent, rope_key, latent_gain, key_up, value_up, out_gain, out_weight, norm_gain, ff_in, ff_out):
    positions = jnp.arange(TOKENS, dtype=jnp.float32)
    lat_full = latent.astype(jnp.float32)
    normed = (lat_full * lax.rsqrt(lax.optimization_barrier(jnp.mean(lat_full * lat_full, axis=-1, keepdims=True)) + EPS) * latent_gain.astype(jnp.float32)).astype(jnp.bfloat16)
    keys_rot = turn(rope_key, positions).astype(jnp.bfloat16)
    query_rot = turn(query_rope, positions).astype(jnp.bfloat16)
    query_lat = jnp.einsum('thn,lhn->thl', query_nope.astype(jnp.float32), key_up.astype(jnp.float32)).astype(jnp.bfloat16)
    score_scale = 1.0 / math.sqrt(NOPE + ROPE)
    normed_wide = normed.astype(jnp.float32)
    keys_wide = keys_rot.astype(jnp.float32)

    def attend(inputs):
        lat_query, rot_query = inputs
        scores = (jnp.einsum('thl,kl->thk', lat_query.astype(jnp.float32), normed_wide) + jnp.einsum('thr,kr->thk', rot_query.astype(jnp.float32), keys_wide)) * score_scale
        row_max = lax.optimization_barrier(jnp.max(scores, axis=-1, keepdims=True))
        expo = jnp.exp(scores - row_max)
        denom = lax.optimization_barrier(jnp.sum(expo, axis=-1))
        probs = lax.optimization_barrier(expo.astype(jnp.bfloat16)).astype(jnp.float32)
        summed = jnp.einsum('thk,kl->thl', probs, normed_wide)
        return (summed / denom[..., None]).astype(jnp.bfloat16)
    q_block = math.gcd(TOKENS, 512)
    out_lat = lax.map(attend, (query_lat.reshape(TOKENS // q_block, q_block, HEADS, LATENT), query_rot.reshape(TOKENS // q_block, q_block, HEADS, ROPE)))
    out_lat = out_lat.reshape(TOKENS, HEADS, LATENT)
    head_out = jnp.einsum('thl,lhv->thv', out_lat.astype(jnp.float32), value_up.astype(jnp.float32))
    row_scale = lax.rsqrt(lax.optimization_barrier(jnp.mean(head_out * head_out, axis=(1, 2))) + EPS)
    gated = (head_out.reshape(TOKENS, HEADS * VDIM) * out_gain.astype(jnp.float32)).astype(jnp.bfloat16)
    mid_stream = stream.astype(jnp.float32) + row_scale[:, None] * jnp.dot(gated, out_weight, preferred_element_type=jnp.float32)
    ff_input = (mid_stream * lax.rsqrt(lax.optimization_barrier(jnp.mean(mid_stream * mid_stream, axis=-1, keepdims=True)) + EPS) * norm_gain.astype(jnp.float32)).astype(jnp.bfloat16)
    pre_act = jnp.dot(ff_input, ff_in, preferred_element_type=jnp.float32)
    activation = jnp.square(jax.nn.relu(pre_act)).astype(jnp.bfloat16)
    return (mid_stream + jnp.dot(activation, ff_out, preferred_element_type=jnp.float32)).astype(jnp.bfloat16)
```

```python
import functools
import math

import jax
import jax.numpy as jnp
from jax import lax
from jax.experimental import pallas as pl
from jax.experimental.pallas import tpu as pltpu
from jax.sharding import PartitionSpec as P

EPS = 1e-06
THETA = 10000.0
F32 = jnp.float32
BF16 = jnp.bfloat16
MESH = pl.DeviceIdType.MESH
LANES = 128


def turn(values, positions):
    full_width = values.shape[-1]
    half_width = full_width // 2
    inverse = jnp.power(THETA, -jnp.arange(0, full_width, 2, dtype=F32) / full_width)
    angles = positions[:, None] * inverse[None, :]
    cosine = jnp.cos(angles)
    sine_part = jnp.sin(angles)
    if values.ndim == 3:
        cosine = cosine[:, None, :]
        sine_part = sine_part[:, None, :]
    vector = values.astype(F32)
    lower_half = vector[..., :half_width]
    upper_half = vector[..., half_width:]
    return jnp.concatenate(
        [
            lower_half * cosine - upper_half * sine_part,
            lower_half * sine_part + upper_half * cosine,
        ],
        axis=-1,
    )


def ring_shape(n):
    rows = 1
    while rows * rows < n:
        rows *= 2
    return (rows, n // rows) if n % rows == 0 else (n, 1)


def ring_pos(n, index):
    nz, ny = ring_shape(n)
    if ny == 1:
        return index
    z, y = index // ny, index % ny
    r = nz - 1 - z
    odd = r % 2
    c = (1 - odd) * (y - 1) + odd * (ny - 1 - y)
    return jnp.where(y == 0, z, nz + r * (ny - 1) + c)


def ring_at(n, pos):
    nz, ny = ring_shape(n)
    if ny == 1:
        return pos
    q = jnp.maximum(pos - nz, 0)
    r, c = q // (ny - 1), q % (ny - 1)
    odd = r % 2
    y = 1 + (1 - odd) * c + odd * (ny - 2 - c)
    return jnp.where(pos < nz, pos * ny, (nz - 1 - r) * ny + y)


def kernel(
    n, tp, heads, latent_width, width,
    kv_ref, q_ref, vup_ref, gain_ref, ow_ref, stream_ref, ngain_ref, ffin_ref, ffout_ref,
    out_ref,
    kv, fi, fo, ow, sc, acc, gated, proj, red, sq_out, sq_in, mid, xs, act, mixed, mix_out, mix_in,
    local_sem, lat_send, lat_recv, par_send, par_recv, w_send, w_recv,
    t_send, t_recv, m_send, m_recv,
):
    sp = lax.axis_index("sp")
    me = lax.axis_index("tp")
    pos = ring_pos(n, sp)
    rows = stream_ref.shape[0] * tp
    share = rows // tp
    total = width
    hidden = act.shape[1]
    dblk = total // n
    keys = kv.shape[0]
    core = me % 2
    partner = me + 1 - 2 * core

    def at(offset):
        return ring_at(n, lax.rem(pos + offset + n, n))

    right, left = at(1), at(-1)
    towards = (right, left)

    def peer(j):
        return lax.rem(me + j, tp)

    local = [
        pltpu.make_async_copy(ffin_ref, fi.at[pl.ds(sp * dblk, dblk)], local_sem.at[0]),
        pltpu.make_async_copy(ffout_ref, fo.at[sp], local_sem.at[1]),
        pltpu.make_async_copy(ow_ref, ow, local_sem.at[2]),
        pltpu.make_async_copy(kv_ref, kv.at[pl.ds(sp * rows, rows)], local_sem.at[3]),
    ]
    for c in (3, 0, 1, 2):
        local[c].start()

    barrier = pltpu.get_barrier_semaphore()
    for d in towards:
        pl.semaphore_signal(barrier, inc=1, device_id=(d, me), device_id_type=MESH)
    for j in range(1, tp):
        pl.semaphore_signal(barrier, inc=1, device_id=(sp, peer(j)), device_id_type=MESH)
    pl.semaphore_wait(barrier, tp + 1)

    quarter = rows // 4

    def lat_piece(src, way, c):
        return kv.at[pl.ds(src * rows + (2 * c + way) * quarter, quarter)]

    def came(way, step):
        return at(-1 - step) if way == 0 else at(1 + step)

    def going(way, step):
        return at(-step) if way == 0 else at(step)

    def lat_copy(way, step):
        ref = lat_piece(going(way, step), way, core)
        return pltpu.make_async_remote_copy(
            ref, ref, lat_send.at[way, step], lat_recv.at[way, step],
            device_id=(towards[way], me), device_id_type=MESH)

    def lat_wait(way, step):
        ref = lat_piece(came(way, step), way, core)
        pltpu.make_async_remote_copy(
            ref, ref, lat_send.at[way, step], lat_recv.at[way, step],
            device_id=(towards[way], me), device_id_type=MESH).wait_recv()

    def par_copy(way, step, c):
        ref = lat_piece(came(way, step), way, c)
        return pltpu.make_async_remote_copy(
            ref, ref, par_send.at[way, step], par_recv.at[way, step],
            device_id=(sp, partner), device_id_type=MESH)

    def w_piece(buf, src, way, sub):
        if buf == 0:
            part = dblk // 4
            return fi.at[pl.ds(src * dblk + (2 * way + sub) * part, part)]
        part = hidden // 4
        return fo.at[src, pl.ds((2 * way + sub) * part, part)]

    def w_copy(buf, way, sub, step):
        ref = w_piece(buf, going(way, step), way, sub)
        return pltpu.make_async_remote_copy(
            ref, ref, w_send.at[buf, way, sub, step], w_recv.at[buf, way, sub, step],
            device_id=(towards[way], me), device_id_type=MESH)

    def w_wait(buf, way, sub, step):
        ref = w_piece(buf, came(way, step), way, sub)
        pltpu.make_async_remote_copy(
            ref, ref, w_send.at[buf, way, sub, step], w_recv.at[buf, way, sub, step],
            device_id=(towards[way], me), device_id_type=MESH).wait_recv()

    def advance(buf, step):
        for sub in range(2):
            for way in range(2):
                if step > 0:
                    w_wait(buf, way, sub, step - 1)
                if step < n - 1:
                    w_copy(buf, way, sub, step).start()

    local[3].wait()
    for way in range(2):
        lat_copy(way, 0).start()
    local[0].wait()
    local[1].wait()
    for step in range(n - 1):
        for way in range(2):
            lat_wait(way, step)
            if step < n - 2:
                lat_copy(way, step + 1).start()
            par_copy(way, step, core).start()
        if step == n - 3:
            advance(0, 0)
    for step in range(n - 1):
        for way in range(2):
            par_copy(way, step, 1 - core).wait_recv()

    hops = [(0, s) for s in range(1, n)] + [(1, s) for s in range(0, n)]
    cursor = [0]

    def hop():
        buf, step = hops[cursor[0]]
        if buf == 0 and step == n - 1:
            cursor[0] += 1
            advance(1, 0)
            advance(0, n - 1)
            cursor[0] += 1
            return
        advance(buf, step)
        cursor[0] += 1

    scale = 1.0 / math.sqrt(LANES + (q_ref.shape[2] - latent_width) // 2)
    chunk = sc.shape[2]
    chunks = keys // chunk
    vdim = LANES
    squares = jnp.zeros((rows, 1), F32)
    fi_hops = n - 1
    points = 2 * heads
    for h in range(heads):
        def score(c, top):
            s = lax.dot_general(
                q_ref[h], kv[pl.ds(c * chunk, chunk), :], (((1,), (1,)), ((), ())),
                preferred_element_type=F32) * scale
            sc[c] = s
            return jnp.maximum(top, jnp.max(s, axis=1, keepdims=True))

        top = lax.fori_loop(0, chunks, score, jnp.full((rows, 1), -jnp.inf, F32))
        if cursor[0] < fi_hops - 1:
            hop()
        acc[...] = jnp.zeros_like(acc)

        def gather(c, den):
            e = jnp.exp(sc[c] - top)
            acc[...] += jnp.dot(
                e.astype(BF16), kv[pl.ds(c * chunk, chunk), pl.ds(0, latent_width)],
                preferred_element_type=F32)
            return den + jnp.sum(e, axis=1, keepdims=True)

        den = lax.fori_loop(0, chunks, gather, jnp.zeros((rows, 1), F32))
        lat = (acc[...] / den).astype(BF16)
        one = jnp.dot(lat, vup_ref[:, h * vdim:(h + 1) * vdim], preferred_element_type=F32)
        squares = squares + jnp.sum(one * one, axis=1, keepdims=True)
        gated[:, h * vdim:(h + 1) * vdim] = (one * gain_ref[:, h * vdim:(h + 1) * vdim]).astype(BF16)
        if cursor[0] < fi_hops - 1:
            hop()
    sq_out[...] = jnp.broadcast_to(squares, sq_out.shape)
    local[2].wait()

    tile = total // 4

    @pl.loop(0, 4)
    def _(c):
        cols = pl.ds(pl.multiple_of(c * tile, tile), tile)
        proj[:, cols] = jnp.dot(gated[...], ow[:, cols], preferred_element_type=F32).astype(BF16)

    def block(owner):
        return pl.ds(owner * share, share)

    def t_copy(kind, j, out):
        other = peer(j) if out else me
        mine = me if out else peer(tp - j)
        if kind == 0:
            a, b = sq_out.at[block(other)], sq_in.at[mine]
        elif kind == 1:
            a, b = proj.at[block(other)], red.at[mine]
        else:
            a = b = xs.at[block(mine)]
        return pltpu.make_async_remote_copy(
            a, b, t_send.at[kind, j], t_recv.at[kind, j],
            device_id=(sp, peer(j)), device_id_type=MESH)

    for j in range(1, tp):
        t_copy(0, j, True).start()
        t_copy(1, j, True).start()
    while cursor[0] < fi_hops - 1:
        hop()
    for j in range(1, tp):
        t_copy(0, j, False).wait_recv()
        t_copy(1, j, False).wait_recv()
    summed = proj[block(me), :].astype(F32)
    square = sq_out[block(me), :]
    for j in range(1, tp):
        summed = summed + red[peer(tp - j)].astype(F32)
        square = square + sq_in[peer(tp - j)]
    row_scale = lax.rsqrt(square[:, :1] / (heads * tp * vdim) + EPS)
    middle = stream_ref[...].astype(F32) + row_scale * summed
    mid[...] = middle
    norm = lax.rsqrt(jnp.mean(middle * middle, axis=1, keepdims=True) + EPS)
    xs[block(me), :] = (middle * norm * ngain_ref[...]).astype(BF16)
    for j in range(1, tp):
        t_copy(2, j, True).start()
    hop()
    for j in range(1, tp):
        t_copy(2, j, False).wait_recv()

    wide = 512 if hidden % 512 == 0 else 128

    def first(c):
        cols = pl.ds(pl.multiple_of(c * wide, wide), wide)
        pre = jnp.dot(xs[...], fi[:, cols], preferred_element_type=F32)
        pre = jnp.maximum(pre, 0.0)
        act[:, cols] = (pre * pre).astype(BF16)

    tiles = hidden // wide
    pl.loop(0, tiles // 2)(first)
    advance(1, 1)
    pl.loop(tiles // 2, tiles)(first)

    mixed[sp] = jnp.dot(act[...], fo[sp], preferred_element_type=F32)
    half = hidden // 2

    def part(src, way):
        return jnp.dot(act[:, way * half:(way + 1) * half], fo[src, way * half:(way + 1) * half],
                       preferred_element_type=F32)

    def m_copy(order, src, j, out):
        other = peer(j) if out else me
        mine = me if out else peer(tp - j)
        return pltpu.make_async_remote_copy(
            mix_out.at[src, block(other)], mix_in.at[mine, src],
            m_send.at[order, j], m_recv.at[order, j],
            device_id=(sp, peer(j)), device_id_type=MESH)

    finished = []
    seen = set()

    def finish(offset, src):
        order = len(finished)
        finished.append(src)
        mix_out[src] = mixed[src].astype(BF16)
        for j in range(1, tp):
            m_copy(order, src, j, True).start()

    for step in range(n - 1):
        if step > 0:
            advance(1, step + 1)
        for way in range(2):
            offset = (-1 - step) % n if way == 0 else (1 + step) % n
            src = came(way, step)
            if offset in seen:
                mixed[src] += part(src, way)
                finish(offset, src)
            else:
                seen.add(offset)
                mixed[src] = part(src, way)
        if step == 0:
            finish(0, sp)

    for order, src in enumerate(finished):
        cols = pl.ds(pl.multiple_of(src * dblk, dblk), dblk)
        whole = mix_out[src, block(me), :].astype(F32)
        for j in range(1, tp):
            m_copy(order, src, j, False).wait_recv()
            whole = whole + mix_in[peer(tp - j), src].astype(F32)
        out_ref[:, cols] = (mid[:, cols] + whole).astype(BF16)

    for step in range(n - 1):
        for way in range(2):
            lat_copy(way, step).wait_send()
            par_copy(way, step, core).wait_send()
            for buf in range(2):
                for sub in range(2):
                    w_copy(buf, way, sub, step).wait_send()
    for j in range(1, tp):
        for kind in range(3):
            t_copy(kind, j, True).wait_send()
        for order, src in enumerate(finished):
            m_copy(order, src, j, True).wait_send()


def body(
    n, tp,
    stream, query_nope, query_rope, latent, rope_key, latent_gain,
    key_up, value_up, out_gain, out_weight, norm_gain, ff_in, ff_out,
):
    rows, heads = query_nope.shape[:2]
    width = stream.shape[1]
    latent_width = latent.shape[1]
    rope = rope_key.shape[1]
    pad = -rope % LANES
    dblk, hidden = ff_in.shape
    share = rows // tp
    positions = (lax.axis_index("sp") * rows + jnp.arange(rows, dtype=jnp.int32)).astype(F32)
    lat_full = latent.astype(F32)
    normed = (
        lat_full
        * lax.rsqrt(jnp.mean(lat_full * lat_full, axis=-1, keepdims=True) + EPS)
        * latent_gain
    ).astype(BF16)
    keys_rot = turn(rope_key, positions).astype(BF16)
    query_rot = turn(query_rope, positions).astype(BF16)
    query_lat = jnp.einsum(
        "thn,lhn->htl", query_nope, key_up, preferred_element_type=F32
    ).astype(BF16)
    kv = jnp.concatenate([normed, keys_rot, jnp.zeros((rows, pad), BF16)], axis=1)
    q = jnp.concatenate(
        [query_lat, query_rot.transpose(1, 0, 2), jnp.zeros((heads, rows, pad), BF16)], axis=2
    )
    keys = n * rows
    chunk = 2 * rows if n % 2 == 0 else rows
    vm = pl.BlockSpec(memory_space=pltpu.VMEM)
    hbm = pl.BlockSpec(memory_space=pl.ANY)
    dma = pltpu.SemaphoreType.DMA
    return pl.pallas_call(
        functools.partial(kernel, n, tp, heads, latent_width, width),
        out_shape=jax.ShapeDtypeStruct((share, width), BF16),
        in_specs=[hbm, vm, vm, vm, hbm, vm, vm, hbm, hbm],
        out_specs=vm,
        scratch_shapes=[
            pltpu.VMEM((keys, kv.shape[1]), BF16),
            pltpu.VMEM((width, hidden), BF16),
            pltpu.VMEM((n, hidden, dblk), BF16),
            pltpu.VMEM(out_weight.shape, BF16),
            pltpu.VMEM((keys // chunk, rows, chunk), F32),
            pltpu.VMEM((rows, latent_width), F32),
            pltpu.VMEM((rows, out_weight.shape[0]), BF16),
            pltpu.VMEM((rows, width), BF16),
            pltpu.VMEM((tp, share, width), BF16),
            pltpu.VMEM((rows, LANES), F32),
            pltpu.VMEM((tp, share, LANES), F32),
            pltpu.VMEM((share, width), F32),
            pltpu.VMEM((rows, width), BF16),
            pltpu.VMEM((rows, hidden), BF16),
            pltpu.VMEM((n, rows, dblk), F32),
            pltpu.VMEM((n, rows, dblk), BF16),
            pltpu.VMEM((tp, n, share, dblk), BF16),
            dma((4,)),
            dma((2, n - 1)), dma((2, n - 1)), dma((2, n - 1)), dma((2, n - 1)),
            dma((2, 2, 2, n - 1)), dma((2, 2, 2, n - 1)),
            dma((3, tp)), dma((3, tp)),
            dma((n, tp)), dma((n, tp)),
        ],
        compiler_params=pltpu.CompilerParams(
            collective_id=0, has_side_effects=True, vmem_limit_bytes=63 * 1024 * 1024
        ),
    )(
        kv, q, value_up.reshape(latent_width, -1), out_gain[None, :], out_weight,
        stream, norm_gain[None, :], ff_in, ff_out,
    )


def solution(mesh):
    placed = (
        P(("sp", "tp"), None),
        P("sp", "tp", None),
        P("sp", "tp", None),
        P("sp", None),
        P("sp", None),
        P(),
        P(None, "tp", None),
        P(None, "tp", None),
        P("tp"),
        P("tp", None),
        P(),
        P("sp", "tp"),
        P("tp", "sp"),
    )
    return jax.shard_map(
        functools.partial(body, mesh.shape["sp"], mesh.shape["tp"]),
        mesh=mesh, in_specs=placed, out_specs=P(("sp", "tp"), None), check_vma=False
    )
```

```python
import functools
import math

import jax
import jax.numpy as jnp
from jax import lax
from jax.experimental import pallas as pl
from jax.experimental.pallas import tpu as pltpu
from jax.sharding import PartitionSpec as P

EPS = 1e-06
THETA = 10000.0
F32 = jnp.float32
BF16 = jnp.bfloat16
MESH = pl.DeviceIdType.MESH
LANES = 128
SUBS = 4


def turn(values, positions):
    full_width = values.shape[-1]
    half_width = full_width // 2
    inverse = jnp.power(THETA, -jnp.arange(0, full_width, 2, dtype=F32) / full_width)
    angles = positions[:, None] * inverse[None, :]
    cosine = jnp.cos(angles)
    sine_part = jnp.sin(angles)
    if values.ndim == 3:
        cosine = cosine[:, None, :]
        sine_part = sine_part[:, None, :]
    vector = values.astype(F32)
    lower_half = vector[..., :half_width]
    upper_half = vector[..., half_width:]
    return jnp.concatenate(
        [
            lower_half * cosine - upper_half * sine_part,
            lower_half * sine_part + upper_half * cosine,
        ],
        axis=-1,
    )


def ring_shape(n):
    rows = 1
    while rows * rows < n:
        rows *= 2
    return (rows, n // rows) if n % rows == 0 else (n, 1)


def ring_pos(n, index):
    nz, ny = ring_shape(n)
    if ny == 1:
        return index
    z, y = index // ny, index % ny
    r = nz - 1 - z
    odd = r % 2
    c = (1 - odd) * (y - 1) + odd * (ny - 1 - y)
    return jnp.where(y == 0, z, nz + r * (ny - 1) + c)


def ring_at(n, pos):
    nz, ny = ring_shape(n)
    if ny == 1:
        return pos
    q = jnp.maximum(pos - nz, 0)
    r, c = q // (ny - 1), q % (ny - 1)
    odd = r % 2
    y = 1 + (1 - odd) * c + odd * (ny - 2 - c)
    return jnp.where(pos < nz, pos * ny, (nz - 1 - r) * ny + y)


def kernel(
    n, tp, heads, latent_width, width,
    kv_ref, q_ref, vup_ref, gain_ref, ow_ref, stream_ref, ngain_ref, ffin_ref, ffout_ref,
    out_ref,
    kv, fi, fo, ow, sc, acc, gated, proj, red, sq_out, sq_in, mid, xs, act, mixed, mix_out, mix_in,
    local_sem, lat_send, lat_recv, par_send, par_recv, w_send, w_recv,
    t_send, t_recv, m_send, m_recv,
):
    sp = lax.axis_index("sp")
    me = lax.axis_index("tp")
    pos = ring_pos(n, sp)
    rows = stream_ref.shape[0] * tp
    share = rows // tp
    total = width
    hidden = act.shape[1]
    dblk = total // n
    keys = kv.shape[0]
    core = me % 2
    partner = me + 1 - 2 * core

    def at(offset):
        return ring_at(n, lax.rem(pos + offset + n, n))

    right, left = at(1), at(-1)
    towards = (right, left)

    def peer(j):
        return lax.rem(me + j, tp)

    local = [
        pltpu.make_async_copy(ffin_ref, fi.at[pl.ds(sp * dblk, dblk)], local_sem.at[0]),
        pltpu.make_async_copy(ffout_ref, fo.at[sp], local_sem.at[1]),
        pltpu.make_async_copy(ow_ref, ow, local_sem.at[2]),
        pltpu.make_async_copy(kv_ref, kv.at[pl.ds(sp * rows, rows)], local_sem.at[3]),
    ]
    for c in (3, 0, 1, 2):
        local[c].start()

    barrier = pltpu.get_barrier_semaphore()
    for d in towards:
        pl.semaphore_signal(barrier, inc=1, device_id=(d, me), device_id_type=MESH)
    for j in range(1, tp):
        pl.semaphore_signal(barrier, inc=1, device_id=(sp, peer(j)), device_id_type=MESH)
    pl.semaphore_wait(barrier, tp + 1)

    quarter = rows // 4

    def lat_piece(src, way, c):
        return kv.at[pl.ds(src * rows + (2 * c + way) * quarter, quarter)]

    def came(way, step):
        return at(-1 - step) if way == 0 else at(1 + step)

    def going(way, step):
        return at(-step) if way == 0 else at(step)

    def lat_copy(way, step):
        ref = lat_piece(going(way, step), way, core)
        return pltpu.make_async_remote_copy(
            ref, ref, lat_send.at[way, step], lat_recv.at[way, step],
            device_id=(towards[way], me), device_id_type=MESH)

    def lat_wait(way, step):
        ref = lat_piece(came(way, step), way, core)
        pltpu.make_async_remote_copy(
            ref, ref, lat_send.at[way, step], lat_recv.at[way, step],
            device_id=(towards[way], me), device_id_type=MESH).wait_recv()

    def par_copy(way, step, c):
        ref = lat_piece(came(way, step), way, c)
        return pltpu.make_async_remote_copy(
            ref, ref, par_send.at[way, step], par_recv.at[way, step],
            device_id=(sp, partner), device_id_type=MESH)

    def w_piece(buf, src, way, sub):
        if buf == 0:
            part = dblk // (2 * SUBS)
            return fi.at[pl.ds(src * dblk + (SUBS * way + sub) * part, part)]
        part = hidden // (2 * SUBS)
        return fo.at[src, pl.ds((SUBS * way + sub) * part, part)]

    def w_copy(buf, way, sub, step):
        ref = w_piece(buf, going(way, step), way, sub)
        return pltpu.make_async_remote_copy(
            ref, ref, w_send.at[buf, way, sub, step], w_recv.at[buf, way, sub, step],
            device_id=(towards[way], me), device_id_type=MESH)

    def w_wait(buf, way, sub, step):
        ref = w_piece(buf, came(way, step), way, sub)
        pltpu.make_async_remote_copy(
            ref, ref, w_send.at[buf, way, sub, step], w_recv.at[buf, way, sub, step],
            device_id=(towards[way], me), device_id_type=MESH).wait_recv()

    units = [(b, s, u) for b in range(2) for s in range(n - 1) for u in range(SUBS)]
    ff_in_units = (n - 1) * SUBS
    cursor = [0]
    waited = set()

    def need(buf, step, sub):
        if (buf, step, sub) not in waited:
            waited.add((buf, step, sub))
            for way in range(2):
                w_wait(buf, way, sub, step)

    def advance(until):
        while cursor[0] < min(until, len(units)):
            buf, step, sub = units[cursor[0]]
            if step > 0:
                need(buf, step - 1, sub)
            for way in range(2):
                w_copy(buf, way, sub, step).start()
            cursor[0] += 1

    def one_more(limit):
        if cursor[0] < limit:
            advance(cursor[0] + 1)

    local[3].wait()
    for way in range(2):
        lat_copy(way, 0).start()
    local[0].wait()
    advance(1)
    for step in range(n - 1):
        for way in range(2):
            lat_wait(way, step)
            if step < n - 2:
                lat_copy(way, step + 1).start()
            par_copy(way, step, core).start()
        one_more(ff_in_units)
    for step in range(n - 1):
        for way in range(2):
            par_copy(way, step, 1 - core).wait_recv()

    scale = 1.0 / math.sqrt(LANES + (q_ref.shape[2] - latent_width) // 2)
    chunk = sc.shape[2]
    chunks = keys // chunk
    vdim = LANES
    squares = jnp.zeros((rows, 1), F32)
    for h in range(heads):
        def score(c, top):
            s = lax.dot_general(
                q_ref[h], kv[pl.ds(c * chunk, chunk), :], (((1,), (1,)), ((), ())),
                preferred_element_type=F32) * scale
            sc[c] = s
            return jnp.maximum(top, jnp.max(s, axis=1, keepdims=True))

        top = lax.fori_loop(0, chunks, score, jnp.full((rows, 1), -jnp.inf, F32))
        one_more(ff_in_units)
        acc[...] = jnp.zeros_like(acc)

        def gather(c, den):
            e = jnp.exp(sc[c] - top)
            acc[...] += jnp.dot(
                e.astype(BF16), kv[pl.ds(c * chunk, chunk), pl.ds(0, latent_width)],
                preferred_element_type=F32)
            return den + jnp.sum(e, axis=1, keepdims=True)

        den = lax.fori_loop(0, chunks, gather, jnp.zeros((rows, 1), F32))
        lat = (acc[...] / den).astype(BF16)
        one = jnp.dot(lat, vup_ref[:, h * vdim:(h + 1) * vdim], preferred_element_type=F32)
        squares = squares + jnp.sum(one * one, axis=1, keepdims=True)
        gated[:, h * vdim:(h + 1) * vdim] = (one * gain_ref[:, h * vdim:(h + 1) * vdim]).astype(BF16)
        one_more(ff_in_units)
    sq_out[...] = jnp.broadcast_to(squares, sq_out.shape)
    local[2].wait()

    tile = total // 4

    def project(c):
        cols = pl.ds(pl.multiple_of(c * tile, tile), tile)
        proj[:, cols] = jnp.dot(gated[...], ow[:, cols], preferred_element_type=F32).astype(BF16)

    pl.loop(0, 2)(project)
    one_more(ff_in_units)
    pl.loop(2, 4)(project)

    def block(owner):
        return pl.ds(owner * share, share)

    def t_copy(kind, j, out):
        other = peer(j) if out else me
        mine = me if out else peer(tp - j)
        if kind == 0:
            a, b = sq_out.at[block(other)], sq_in.at[mine]
        elif kind == 1:
            a, b = proj.at[block(other)], red.at[mine]
        else:
            a = b = xs.at[block(mine)]
        return pltpu.make_async_remote_copy(
            a, b, t_send.at[kind, j], t_recv.at[kind, j],
            device_id=(sp, peer(j)), device_id_type=MESH)

    for j in range(1, tp):
        t_copy(0, j, True).start()
        t_copy(1, j, True).start()
    advance(ff_in_units - SUBS - 2)
    for j in range(1, tp):
        t_copy(0, j, False).wait_recv()
        t_copy(1, j, False).wait_recv()
    summed = proj[block(me), :].astype(F32)
    square = sq_out[block(me), :]
    for j in range(1, tp):
        summed = summed + red[peer(tp - j)].astype(F32)
        square = square + sq_in[peer(tp - j)]
    row_scale = lax.rsqrt(square[:, :1] / (heads * tp * vdim) + EPS)
    middle = stream_ref[...].astype(F32) + row_scale * summed
    mid[...] = middle
    norm = lax.rsqrt(jnp.mean(middle * middle, axis=1, keepdims=True) + EPS)
    xs[block(me), :] = (middle * norm * ngain_ref[...]).astype(BF16)
    for j in range(1, tp):
        t_copy(2, j, True).start()
    local[1].wait()
    advance(ff_in_units + SUBS)
    for sub in range(SUBS):
        need(0, n - 2, sub)
    for j in range(1, tp):
        t_copy(2, j, False).wait_recv()

    wide = 512 if hidden % 512 == 0 else 128

    def first(c):
        cols = pl.ds(c * wide, wide)
        pre = jnp.dot(xs[...], fi[:, cols], preferred_element_type=F32)
        pre = jnp.maximum(pre, 0.0)
        act[:, cols] = (pre * pre).astype(BF16)

    for c in range(hidden // wide):
        first(c)
        one_more(len(units))

    mixed[sp] = jnp.dot(act[...], fo[sp], preferred_element_type=F32)
    half = hidden // 2

    def part(src, way):
        return jnp.dot(act[:, way * half:(way + 1) * half], fo[src, way * half:(way + 1) * half],
                       preferred_element_type=F32)

    def m_copy(order, src, j, out):
        other = peer(j) if out else me
        mine = me if out else peer(tp - j)
        return pltpu.make_async_remote_copy(
            mix_out.at[src, block(other)], mix_in.at[mine, src],
            m_send.at[order, j], m_recv.at[order, j],
            device_id=(sp, peer(j)), device_id_type=MESH)

    finished = []
    seen = set()

    def finish(offset, src):
        order = len(finished)
        finished.append(src)
        mix_out[src] = mixed[src].astype(BF16)
        for j in range(1, tp):
            m_copy(order, src, j, True).start()

    for step in range(n - 1):
        advance(ff_in_units + (step + 2) * SUBS)
        for sub in range(SUBS):
            need(1, step, sub)
        for way in range(2):
            offset = (-1 - step) % n if way == 0 else (1 + step) % n
            src = came(way, step)
            if offset in seen:
                mixed[src] += part(src, way)
                finish(offset, src)
            else:
                seen.add(offset)
                mixed[src] = part(src, way)
        if step == 0:
            finish(0, sp)

    for order, src in enumerate(finished):
        cols = pl.ds(pl.multiple_of(src * dblk, dblk), dblk)
        whole = mix_out[src, block(me), :].astype(F32)
        for j in range(1, tp):
            m_copy(order, src, j, False).wait_recv()
            whole = whole + mix_in[peer(tp - j), src].astype(F32)
        out_ref[:, cols] = (mid[:, cols] + whole).astype(BF16)

    for step in range(n - 1):
        for way in range(2):
            lat_copy(way, step).wait_send()
            par_copy(way, step, core).wait_send()
            for buf in range(2):
                for sub in range(SUBS):
                    w_copy(buf, way, sub, step).wait_send()
    for j in range(1, tp):
        for kind in range(3):
            t_copy(kind, j, True).wait_send()
        for order, src in enumerate(finished):
            m_copy(order, src, j, True).wait_send()


def body(
    n, tp,
    stream, query_nope, query_rope, latent, rope_key, latent_gain,
    key_up, value_up, out_gain, out_weight, norm_gain, ff_in, ff_out,
):
    rows, heads = query_nope.shape[:2]
    width = stream.shape[1]
    latent_width = latent.shape[1]
    rope = rope_key.shape[1]
    pad = -rope % LANES
    dblk, hidden = ff_in.shape
    share = rows // tp
    positions = (lax.axis_index("sp") * rows + jnp.arange(rows, dtype=jnp.int32)).astype(F32)
    lat_full = latent.astype(F32)
    normed = (
        lat_full
        * lax.rsqrt(jnp.mean(lat_full * lat_full, axis=-1, keepdims=True) + EPS)
        * latent_gain
    ).astype(BF16)
    keys_rot = turn(rope_key, positions).astype(BF16)
    query_rot = turn(query_rope, positions).astype(BF16)
    query_lat = jnp.einsum(
        "thn,lhn->htl", query_nope, key_up, preferred_element_type=F32
    ).astype(BF16)
    kv = jnp.concatenate([normed, keys_rot, jnp.zeros((rows, pad), BF16)], axis=1)
    q = jnp.concatenate(
        [query_lat, query_rot.transpose(1, 0, 2), jnp.zeros((heads, rows, pad), BF16)], axis=2
    )
    keys = n * rows
    chunk = 2 * rows if n % 2 == 0 else rows
    vm = pl.BlockSpec(memory_space=pltpu.VMEM)
    hbm = pl.BlockSpec(memory_space=pl.ANY)
    dma = pltpu.SemaphoreType.DMA
    return pl.pallas_call(
        functools.partial(kernel, n, tp, heads, latent_width, width),
        out_shape=jax.ShapeDtypeStruct((share, width), BF16),
        in_specs=[hbm, vm, vm, vm, hbm, vm, vm, hbm, hbm],
        out_specs=vm,
        scratch_shapes=[
            pltpu.VMEM((keys, kv.shape[1]), BF16),
            pltpu.VMEM((width, hidden), BF16),
            pltpu.VMEM((n, hidden, dblk), BF16),
            pltpu.VMEM(out_weight.shape, BF16),
            pltpu.VMEM((keys // chunk, rows, chunk), F32),
            pltpu.VMEM((rows, latent_width), F32),
            pltpu.VMEM((rows, out_weight.shape[0]), BF16),
            pltpu.VMEM((rows, width), BF16),
            pltpu.VMEM((tp, share, width), BF16),
            pltpu.VMEM((rows, LANES), F32),
            pltpu.VMEM((tp, share, LANES), F32),
            pltpu.VMEM((share, width), F32),
            pltpu.VMEM((rows, width), BF16),
            pltpu.VMEM((rows, hidden), BF16),
            pltpu.VMEM((n, rows, dblk), F32),
            pltpu.VMEM((n, rows, dblk), BF16),
            pltpu.VMEM((tp, n, share, dblk), BF16),
            dma((4,)),
            dma((2, n - 1)), dma((2, n - 1)), dma((2, n - 1)), dma((2, n - 1)),
            dma((2, 2, SUBS, n - 1)), dma((2, 2, SUBS, n - 1)),
            dma((3, tp)), dma((3, tp)),
            dma((n, tp)), dma((n, tp)),
        ],
        compiler_params=pltpu.CompilerParams(
            collective_id=0, has_side_effects=True, vmem_limit_bytes=63 * 1024 * 1024
        ),
    )(
        kv, q, value_up.reshape(latent_width, -1), out_gain[None, :], out_weight,
        stream, norm_gain[None, :], ff_in, ff_out,
    )


def solution(mesh):
    placed = (
        P(("sp", "tp"), None),
        P("sp", "tp", None),
        P("sp", "tp", None),
        P("sp", None),
        P("sp", None),
        P(),
        P(None, "tp", None),
        P(None, "tp", None),
        P("tp"),
        P("tp", None),
        P(),
        P("sp", "tp"),
        P("tp", "sp"),
    )
    return jax.shard_map(
        functools.partial(body, mesh.shape["sp"], mesh.shape["tp"]),
        mesh=mesh, in_specs=placed, out_specs=P(("sp", "tp"), None), check_vma=False
    )
```
